128 devices in a mesh: fs: 16 (over z, y), tp: 8 (over x, core).
Axes of the slice: x: 4, y: 4, z: 4, core: 2. Of those that a mesh axis runs over, the one named last changes fastest.
Arguments:
- tokens: bfloat16 [16384, 2048], P('fs', 'tp'), may hold values from -6 to 6
- mix_gain: float32 [2048], replicated, may hold values from 0.1 to 1.9
- in_weight: float32 [2048, 1024], P('fs', 'tp'), may hold values from -0.125 to 0.125
- in_scale: float32 [1024], P('tp'), may hold values from 0.4 to 2.5
- out_weight: float32 [1024, 2048], P('tp', 'fs'), may hold values from -0.1875 to 0.1875
- out_scale: float32 [2048], P('fs'), may hold values from 0.4 to 2.5
- ffn_gain: float32 [2048], replicated, may hold values from 0.1 to 1.9
- gate_weight: float32 [2048, 6144], P('fs', 'tp'), may hold values from -0.125 to 0.125
- gate_scale: float32 [6144], P('tp'), may hold values from 0.4 to 2.5
- up_weight: float32 [2048, 6144], P('fs', 'tp'), may hold values from -0.125 to 0.125
- up_scale: float32 [6144], P('tp'), may hold values from 0.4 to 2.5
- down_weight: float32 [6144, 2048], P('tp', 'fs'), may hold values from -0.078125 to 0.078125
- down_scale: float32 [2048], P('fs'), may hold values from 0.4 to 2.5
Outputs:
- layer_out: bfloat16 [16384, 2048], P('fs', 'tp')
The draws below stay inside these ranges and needn't reach their ends.
All inputs are finite; a program needn't handle non-finite values.
Results may differ from the reference program's by a relative error of at most 0.023.
Values may be sent and summed in bfloat16 or wider, within the bound.
No kernel may reach another device: no remote copies, remote signals or barrier semaphores. Data moves between devices by JAX's collectives and lax.ppermute only.
A program may use at most 128 MiB of HBM per device.

```python
import math
import jax
import jax.numpy as jnp
from jax import lax

D = 2048
PW = 1024
FF = 6144
GROUPS = 4
GRID_W = 64
ROWS = 16
TOKENS = 16384
GC = 256
PW_DEV = 128
FF_DEV = 768


def levels(key, shape, cuts, smallest, top_value):
    loudness = 1.0
    for axis_at, blocks in cuts:
        steps = jax.random.uniform(jax.random.fold_in(jax.random.fold_in(key, 6), axis_at), (blocks,), jnp.float32, smallest / len(cuts), top_value / len(cuts))
        loudness = loudness * jnp.repeat(jnp.exp(steps), shape[axis_at] // blocks).reshape((-1,) + (1,) * (len(shape) - 1 - axis_at))
    return loudness


def centred(stream_key, dims, width, most, split=(), kind=jnp.bfloat16):
    level = levels(stream_key, dims, split, -0.22, 0.18) if split else 1.0
    result = jax.random.normal(stream_key, dims, jnp.float32) * width * level
    return jnp.minimum(jnp.maximum(result, -most), most).astype(kind)


def setup_inputs(seed: int = 0) -> dict:
    splits = jax.random.split(jax.random.key(seed), 14)
    return {
        "tokens": centred(splits[0], (TOKENS, D), 1.0, 6.0, ((0, 16), (1, 8))),
        "mix_gain": jnp.clip(1.0 + 0.18 * jax.random.normal(splits[1], (D,), jnp.float32), 0.1, 1.9),
        "in_weight": centred(splits[2], (D, PW), D ** -0.5, 0.125, ((0, 16), (1, 8)), jnp.float32),
        "in_scale": jnp.clip(jnp.exp(math.log(2.5) - 1.8325814 * jax.random.uniform(splits[3], (PW,), jnp.float32) ** levels(splits[3], (PW,), ((0, 8),), -0.2, 0.2)), 0.4, 2.5),
        "out_weight": centred(splits[4], (PW, D), PW ** -0.5, 0.1875, ((0, 8), (1, 16)), jnp.float32),
        "out_scale": jnp.clip(jnp.exp(math.log(2.5) - 1.8325814 * jax.random.uniform(splits[5], (D,), jnp.float32) ** levels(splits[5], (D,), ((0, 16),), -0.2, 0.2)), 0.4, 2.5),
        "ffn_gain": jnp.clip(1.0 + 0.18 * jax.random.normal(splits[6], (D,), jnp.float32), 0.1, 1.9),
        "gate_weight": centred(splits[7], (D, FF), D ** -0.5, 0.125, ((0, 16), (1, 8)), jnp.float32),
        "gate_scale": jnp.clip(jnp.exp(math.log(2.5) - 1.8325814 * jax.random.uniform(splits[8], (FF,), jnp.float32) ** levels(splits[8], (FF,), ((0, 8),), -0.2, 0.2)), 0.4, 2.5),
        "up_weight": centred(splits[9], (D, FF), D ** -0.5, 0.125, ((0, 16), (1, 8)), jnp.float32),
        "up_scale": jnp.clip(jnp.exp(math.log(2.5) - 1.8325814 * jax.random.uniform(splits[10], (FF,), jnp.float32) ** levels(splits[10], (FF,), ((0, 8),), -0.2, 0.2)), 0.4, 2.5),
        "down_weight": centred(splits[11], (FF, D), FF ** -0.5, 0.078125, ((0, 8), (1, 16)), jnp.float32),
        "down_scale": jnp.clip(jnp.exp(math.log(2.5) - 1.8325814 * jax.random.uniform(splits[12], (D,), jnp.float32) ** levels(splits[12], (D,), ((0, 16),), -0.2, 0.2)), 0.4, 2.5),
    }


WINDOWS = (2, 4, 8, 16)
EPSILON = 1e-06

def box_mean(values, window, along):
    length = values.shape[along]
    position = jnp.arange(length, dtype=jnp.int32)
    lower_end = jnp.clip(position - window // 2, 0, length).astype(jnp.int32)
    upper_end = jnp.clip(position + (window - window // 2), 0, length).astype(jnp.int32)
    padding = [(0, 0)] * values.ndim
    padding[along] = (1, 0)
    running = jnp.pad(jnp.cumsum(values, axis=along), padding)
    summed = jnp.take(running, upper_end, axis=along) - jnp.take(running, lower_end, axis=along)
    shaped = [1] * values.ndim
    shaped[along] = length
    return summed / (upper_end - lower_end).astype(jnp.float32).reshape(shaped)

def norm_input(stream, gain):
    inverse_rms = lax.rsqrt(lax.optimization_barrier(jnp.mean(stream * stream, axis=-1, keepdims=True)) + EPSILON)
    return ((stream * gain).astype(jnp.bfloat16), inverse_rms)

def block_sum(hidden, weight, scale, extent):
    total = jnp.zeros((hidden.shape[0], weight.shape[1]), jnp.float32)
    for member in range(hidden.shape[1] // extent):
        term = jnp.dot(hidden[:, member * extent:(member + 1) * extent], weight[member * extent:(member + 1) * extent], preferred_element_type=jnp.float32) * scale
        total = total + term.astype(jnp.bfloat16).astype(jnp.float32)
    return total

def reference(tokens, mix_gain, in_weight, in_scale, out_weight, out_scale, ffn_gain, gate_weight, gate_scale, up_weight, up_scale, down_weight, down_scale):
    stream = tokens.astype(jnp.float32)
    normed, inverse_rms = norm_input(stream, mix_gain)
    channels = jnp.dot(normed, in_weight.astype(jnp.bfloat16), preferred_element_type=jnp.float32) * inverse_rms * in_scale
    lattice = channels.reshape(-1, ROWS, GRID_W, GROUPS, GC)
    differences = []
    for group in range(GROUPS):
        values = lattice[:, :, :, group]
        smoothed = box_mean(box_mean(values, WINDOWS[group], 2), WINDOWS[group], 1)
        differences.append(smoothed - values)
    pooled = jnp.stack(differences, axis=3).reshape(TOKENS, PW).astype(jnp.bfloat16)
    mixed = block_sum(pooled, out_weight.astype(jnp.bfloat16), out_scale, PW_DEV)
    residual = (stream + mixed).astype(jnp.bfloat16)
    normed_ffn, inverse_ffn = norm_input(residual.astype(jnp.float32), ffn_gain)
    gate_value = jnp.dot(normed_ffn, gate_weight.astype(jnp.bfloat16), preferred_element_type=jnp.float32) * inverse_ffn * gate_scale
    up_value = jnp.dot(normed_ffn, up_weight.astype(jnp.bfloat16), preferred_element_type=jnp.float32) * inverse_ffn * up_scale
    hidden = (jax.nn.silu(gate_value) * up_value).astype(jnp.bfloat16)
    channel_out = block_sum(hidden, down_weight.astype(jnp.bfloat16), down_scale, FF_DEV)
    return (residual.astype(jnp.float32) + channel_out).astype(jnp.bfloat16)
```

```python
import functools

import jax
import jax.numpy as jnp
from jax import lax
from jax.experimental import pallas as pl
from jax.experimental.pallas import tpu as pltpu
from jax.sharding import Mesh
from jax.sharding import PartitionSpec as P

D = 2048
GRID_W = 64
ROWS = 16
EPSILON = 1e-06
FS = ("z", "y")
TP = ("x", "c")
SIZES = {"z": 4, "y": 4, "x": 4, "c": 2}
BF16 = jnp.bfloat16
F32 = jnp.float32


Y1, Y2, Z1, Z2 = ("y", 1, 1), ("y", 3, 3), ("z", 1, 4), ("z", 3, 12)


def exchange(value, axis, mask):
    return lax.ppermute(value, axis, [(i, i ^ mask) for i in range(SIZES[axis])])


def doubled(block, order):
    held, masks = block, [0]
    for axis, mask, flat in order[:-1]:
        held = jnp.concatenate([held, exchange(held, axis, mask)], axis=0)
        masks = masks + [m ^ flat for m in masks]
    axis, mask, flat = order[-1]
    return (held, masks), (exchange(held, axis, mask), [m ^ flat for m in masks])


def run_copies(pairs, sems):
    copies = [pltpu.make_async_copy(a, b, sems.at[n]) for n, (a, b) in enumerate(pairs)]
    for copy in copies:
        copy.start()
    for copy in copies:
        copy.wait()


def block_pairs(refs, masks, me, place):
    pairs = []
    for ref, group in zip(refs, masks):
        rows = ref.shape[0] // len(group)
        for n, mask in enumerate(group):
            pairs.append((ref.at[pl.ds(n * rows, rows)], place(me ^ mask)))
    return pairs


def at128(index):
    return pl.ds(pl.multiple_of(index * 128, 128), 128)


def at256(index):
    return pl.ds(pl.multiple_of(index * 256, 256), 256)


HBM = pl.BlockSpec(memory_space=pltpu.HBM)
VMEM = pl.BlockSpec(memory_space=pltpu.VMEM)
SMEM = pl.BlockSpec(memory_space=pltpu.SMEM)


def call(kernel, **kw):
    flops = kw.pop("flops")
    mib = kw.pop("mib", 40)
    return pl.pallas_call(
        kernel,
        compiler_params=pltpu.CompilerParams(vmem_limit_bytes=mib * 1024 * 1024),
        cost_estimate=pl.CostEstimate(flops=flops, bytes_accessed=8 << 20, transcendentals=0),
        **kw,
    )


def split_kernel(masks, me, low, high, in_out, out_out):
    f = me[0]
    for ref, group in zip((low, high), masks):
        for n, mask in enumerate(group):
            there = at128(f ^ mask)
            in_out[there, :] = ref[n * 256 : n * 256 + 128, :]
            out_out[:, there] = ref[n * 256 + 128 : n * 256 + 256, :]


def split_in_out(me, low, high):
    masks = (low[1], high[1])
    return call(
        functools.partial(split_kernel, masks),
        in_specs=[SMEM, VMEM, VMEM],
        out_specs=[VMEM, VMEM],
        out_shape=[
            jax.ShapeDtypeStruct((D, 128), BF16),
            jax.ShapeDtypeStruct((128, D), BF16),
        ],
        flops=1 << 20,
        name="split_in_out",
    )(me, low[0], high[0])


def mixer_kernel(where, me, gain, in_w, in_scale, box, recip, *rest):
    pieces, (pooled, tokens_out, held, ch, sems, out_sem) = rest[:-6], rest[-6:]
    t = me[1]
    pairs = []
    for ref, spots in zip(pieces, where):
        rows = ref.shape[0] // len(spots)
        for n, (mask, row) in enumerate(spots):
            pairs.append(
                (ref.at[pl.ds(n * rows, rows)], held.at[pl.ds(row, rows), at256(t ^ mask)])
            )
    run_copies(pairs, sems)
    out = pltpu.make_async_copy(held, tokens_out, out_sem)
    out.start()

    def step(n, _):
        rows = pl.ds(pl.multiple_of(n * 128, 128), 128)
        x = held[rows, :].astype(F32)
        squares = jnp.sum(x * x, axis=1, keepdims=True)
        scaled = (x * gain[...]).astype(BF16)
        total = jnp.dot(scaled, in_w[...], preferred_element_type=F32)
        ch[rows, :] = total * lax.rsqrt(squares / D + EPSILON) * in_scale[...]
        return 0

    lax.fori_loop(0, 8, step, 0)
    values = ch[...]
    high = values.astype(BF16)
    low = (values - high.astype(F32)).astype(BF16)
    means = jnp.dot(box[...], high, preferred_element_type=F32)
    means = means + jnp.dot(box[...], low, preferred_element_type=F32)
    pooled[...] = (means * recip[...] - values).astype(BF16)
    out.wait()


def mixer(me, gain, in_w, in_scale, box, recip, pieces, where):
    count = sum(len(w) for w in where)
    return call(
        functools.partial(mixer_kernel, where),
        in_specs=[SMEM] + [VMEM] * 5 + [HBM] * len(pieces),
        out_specs=[VMEM, HBM],
        out_shape=[
            jax.ShapeDtypeStruct((1024, 128), BF16),
            jax.ShapeDtypeStruct((1024, D), BF16),
        ],
        scratch_shapes=[
            pltpu.VMEM((1024, D), BF16),
            pltpu.VMEM((1024, 128), F32),
            pltpu.SemaphoreType.DMA((count,)),
            pltpu.SemaphoreType.DMA(()),
        ],
        flops=2 * 1024 * D * 128,
        name="mixer",
    )(me, gain, in_w, in_scale, box, recip, *pieces)


def residual_kernel(me, gain, tokens, *rest):
    pooled = rest[:8]
    weights = rest[8:16]
    normed, inverse, own, w_held, p_held, r_held, sems = rest[16:]

    @pl.when(pl.program_id(0) == 0)
    def _():
        pairs = []
        for n in range(8):
            pairs.append((weights[n], w_held.at[pl.ds(n * 128, 128)]))
            pairs.append((pooled[n], p_held.at[:, pl.ds(n * 128, 128)]))
        run_copies(pairs, sems)

    rows = pl.ds(pl.multiple_of(pl.program_id(0) * 256, 256), 256)
    mixed = jnp.dot(p_held[rows, :], w_held[...], preferred_element_type=F32)
    res = (tokens[...].astype(F32) + mixed).astype(BF16)
    r_held[...] = res
    own[...] = r_held[:, at256(me[1])]
    wide = res.astype(F32)
    squares = jnp.sum(wide * wide, axis=1, keepdims=True)
    inverse[...] = lax.rsqrt(squares / D + EPSILON)
    normed[...] = (wide * gain[...]).astype(BF16)


def residual_of(me, gain, tokens, pooled, weights):
    return call(
        residual_kernel,
        grid=(4,),
        in_specs=[
            SMEM,
            pl.BlockSpec((1, D), lambda i: (0, 0)),
            pl.BlockSpec((256, D), lambda i: (i, 0)),
        ]
        + [HBM] * 16,
        out_specs=[
            pl.BlockSpec((256, D), lambda i: (i, 0)),
            pl.BlockSpec((256, 1), lambda i: (i, 0)),
            pl.BlockSpec((256, 256), lambda i: (i, 0)),
        ],
        out_shape=[
            jax.ShapeDtypeStruct((1024, D), BF16),
            jax.ShapeDtypeStruct((1024, 1), F32),
            jax.ShapeDtypeStruct((1024, 256), BF16),
        ],
        scratch_shapes=[
            pltpu.VMEM((1024, D), BF16),
            pltpu.VMEM((1024, 1024), BF16),
            pltpu.VMEM((256, D), BF16),
            pltpu.SemaphoreType.DMA((16,)),
        ],
        flops=2 * 1024 * 1024 * D,
        name="residual",
    )(me, gain, tokens, *pooled, *weights)


def hidden_kernel(masks, me, normed, inverse, gs, us, g0, g1, u0, u1, hidden, wg, wu, sems):
    @pl.when(pl.program_id(0) == 0)
    def _():
        f = me[0]
        pairs = block_pairs((g0, g1), masks[0], f, lambda b: wg.at[at128(b)])
        pairs += block_pairs((u0, u1), masks[1], f, lambda b: wu.at[at128(b)])
        run_copies(pairs, sems)

    x = normed[...]
    inv = inverse[...]
    gate = jnp.dot(x, wg[...], preferred_element_type=F32) * inv * gs[...]
    up = jnp.dot(x, wu[...], preferred_element_type=F32) * inv * us[...]
    hidden[...] = (gate / (1.0 + jnp.exp(-gate)) * up).astype(BF16)


def hidden_of(me, normed, inverse, gate_scale, up_scale, gate, up):
    masks = ((gate[0][1], gate[1][1]), (up[0][1], up[1][1]))
    return call(
        functools.partial(hidden_kernel, masks),
        grid=(4,),
        in_specs=[
            SMEM,
            pl.BlockSpec((256, D), lambda i: (i, 0)),
            pl.BlockSpec((256, 1), lambda i: (i, 0)),
            pl.BlockSpec((1, 768), lambda i: (0, 0)),
            pl.BlockSpec((1, 768), lambda i: (0, 0)),
        ]
        + [HBM] * 4,
        out_specs=pl.BlockSpec((256, 768), lambda i: (i, 0)),
        out_shape=jax.ShapeDtypeStruct((1024, 768), BF16),
        scratch_shapes=[
            pltpu.VMEM((D, 768), BF16),
            pltpu.VMEM((D, 768), BF16),
            pltpu.SemaphoreType.DMA((32,)),
        ],
        flops=2 * 1024 * 1536 * D,
        name="hidden",
    )(me, normed, inverse, gate_scale, up_scale, gate[0][0], gate[1][0], up[0][0], up[1][0])


def down_kernel(masks, me, hidden, d0, d1, keep, send, wd, sems):
    @pl.when(pl.program_id(0) == 0)
    def _():
        f, t = me[0], me[1]

        def place(b):
            return wd.at[:, at128(((b >> 1) ^ t) * 2 + (b & 1))]

        run_copies(block_pairs((d0, d1), masks, f, place), sems)

    x = hidden[...]
    for m in range(4):
        both = jnp.dot(x, wd[:, m * 512 : m * 512 + 512], preferred_element_type=F32)
        keep[m] = both[:, :256].astype(BF16)
        send[m] = both[:, 256:].astype(BF16)


def down_of(me, hidden, down):
    masks = (down[0][1], down[1][1])
    return call(
        functools.partial(down_kernel, masks),
        grid=(4,),
        in_specs=[SMEM, pl.BlockSpec((256, 768), lambda i: (i, 0)), HBM, HBM],
        out_specs=[pl.BlockSpec((4, 256, 256), lambda i: (0, i, 0))] * 2,
        out_shape=[jax.ShapeDtypeStruct((4, 1024, 256), BF16)] * 2,
        scratch_shapes=[pltpu.VMEM((768, D), BF16), pltpu.SemaphoreType.DMA((16,))],
        flops=2 * 1024 * 768 * D,
        name="down",
    )(me, hidden, down[0][0], down[1][0])


def box_of(x):
    window = jnp.left_shift(2, x)
    half = window // 2

    def inside(p, q):
        return (q >= p - half) & (q < p + (window - half))

    def count(p, length):
        return jnp.minimum(p + (window - half), length) - jnp.maximum(p - half, 0)

    p = lax.broadcasted_iota(jnp.int32, (1024, 1024), 0)
    q = lax.broadcasted_iota(jnp.int32, (1024, 1024), 1)
    box = inside(p // GRID_W, q // GRID_W) & inside(p % GRID_W, q % GRID_W)
    r = lax.broadcasted_iota(jnp.int32, (1024, 1), 0)
    cells = count(r // GRID_W, ROWS) * count(r % GRID_W, GRID_W)
    return box.astype(BF16), 1.0 / cells.astype(F32)


def local(
    tokens,
    mix_gain,
    in_weight,
    in_scale,
    out_weight,
    out_scale,
    ffn_gain,
    gate_weight,
    gate_scale,
    up_weight,
    up_scale,
    down_weight,
    down_scale,
):
    z, y, x, c = (lax.axis_index(a) for a in ("z", "y", "x", "c"))
    me = jnp.stack([z * 4 + y, x * 2 + c]).astype(jnp.int32)

    out_low = (out_weight.astype(BF16).astype(F32) * out_scale).astype(BF16)
    down_low = (down_weight.astype(BF16).astype(F32) * down_scale).astype(BF16)
    in_out = jnp.concatenate([in_weight.astype(BF16), out_low], axis=0)
    in_out = doubled(in_out, (Y1, Z1, Y2, Z2))
    gate = doubled(gate_weight.astype(BF16), (Z1, Y2, Z2, Y1))
    up = doubled(up_weight.astype(BF16), (Y2, Z2, Y1, Z1))
    down = doubled(down_low, (Z2, Y1, Z1, Y2))

    upper, lower = tokens[:512], tokens[512:]
    a1 = exchange(upper, "x", 3)
    b1 = exchange(lower, "x", 1)
    a2 = exchange(jnp.concatenate([upper, a1], axis=0), "x", 1)
    b2 = exchange(jnp.concatenate([lower, b1], axis=0), "x", 3)
    pieces = [tokens, a1, b1, a2, b2]
    where = [[(0, 0)], [(6, 0)], [(2, 512)], [(2, 0), (4, 0)], [(6, 512), (4, 512)]]
    pieces = pieces + [exchange(p, "c", 1) for p in pieces]
    where = where + [[(m ^ 1, r) for m, r in w] for w in where]

    in_full, out_own = split_in_out(me, *in_out)
    box, recip = box_of(x)
    pooled, all_tokens = mixer(
        me, mix_gain[None], in_full, in_scale[None], box, recip, pieces, where
    )

    w_held = [out_own] + [exchange(out_own, "x", m) for m in (1, 3, 2)]
    p_held = [pooled] + [exchange(pooled, "x", m) for m in (1, 3, 2)]
    w_held = w_held + [exchange(w, "c", 1) for w in w_held]
    p_held = p_held + [exchange(p, "c", 1) for p in p_held]
    normed, inverse, residual = residual_of(me, ffn_gain[None], all_tokens, p_held, w_held)

    hidden = hidden_of(me, normed, inverse, gate_scale[None], up_scale[None], gate, up)
    keep, send = down_of(me, hidden, down)

    got = exchange(send, "c", 1)

    def chip_sum(m, rows):
        return keep[m, rows].astype(F32) + got[m, rows].astype(F32)

    ends = []
    for rows, first, second in ((slice(0, 512), 3, 1), (slice(512, 1024), 1, 3)):
        sent = jnp.stack([chip_sum(first, rows), chip_sum(2, rows)]).astype(BF16)
        came = exchange(sent, "x", first).astype(F32)
        last = exchange((chip_sum(second, rows) + came[1]).astype(BF16), "x", second)
        total = chip_sum(0, rows) + came[0] + last.astype(F32)
        ends.append((residual[rows].astype(F32) + total).astype(BF16))
    return jnp.concatenate(ends, axis=0)


def solution(mesh):
    finer = Mesh(mesh.devices.reshape(4, 4, 4, 2), ("z", "y", "x", "c"))
    return jax.shard_map(
        local,
        mesh=finer,
        in_specs=(
            P(FS, TP),
            P(),
            P(FS, TP),
            P(TP),
            P(TP, FS),
            P(FS),
            P(),
            P(FS, TP),
            P(TP),
            P(FS, TP),
            P(TP),
            P(TP, FS),
            P(FS),
        ),
        out_specs=P(FS, TP),
        check_vma=False,
    )
```

```python
import functools

import jax
import jax.numpy as jnp
from jax import lax
from jax.experimental import pallas as pl
from jax.experimental.pallas import tpu as pltpu
from jax.sharding import Mesh
from jax.sharding import PartitionSpec as P

D = 2048
GRID_W = 64
ROWS = 16
EPSILON = 1e-06
FS = ("z", "y")
TP = ("x", "c")
BF16 = jnp.bfloat16
F32 = jnp.float32


BIT = {"ya": 0, "yb": 1, "za": 2, "zb": 3}
ONE = ("ya", "za", "yb", "zb")
TWO = ("za", "yb", "zb", "ya")
THREE = ("yb", "za", "ya", "zb")


def mask_of(step, c):
    if step[1:] == "ab":
        return 2
    return 1 if (step[-1] == "a") == (c == 0) else 3


def cross(value, step):
    axis = step[0]
    pairs = [(i * 2 + c, (i ^ mask_of(step, c)) * 2 + c) for i in range(4) for c in range(2)]
    return lax.ppermute(value, (axis, "c"), pairs)


def swap(value):
    return lax.ppermute(value, "c", [(0, 1), (1, 0)])


def spread(held):
    a = cross(held, "xa")
    b = cross(held, "xb")
    return [held, a, b, cross(a, "xb")]


def places(order):
    return [sum(((p >> k) & 1) << BIT[s] for k, s in enumerate(order)) for p in range(16)]


def position(order, block):
    total = 0
    for k, step in enumerate(order):
        total = total + (((block >> BIT[step]) & 1) << k)
    return total


def xor_of(j, c):
    values = []
    for core in range(2):
        value = 0
        for step, bit in BIT.items():
            if (j >> bit) & 1:
                value ^= mask_of(step, core) * (4 if step[0] == "z" else 1)
        values.append(value)
    return values[0] + c * (values[1] - values[0])


def block_of(xor, c):
    high = (xor >> 1) & 5
    low = (xor ^ (xor >> 1)) & 5
    return jnp.where(c == 0, high * 2 + low, low * 2 + high)


def other_core(j):
    return ((j & 5) << 1) | ((j >> 1) & 5)


def lanes(j):
    return slice(j * 128, j * 128 + 128)


def at128(index):
    return pl.ds(pl.multiple_of(index * 128, 128), 128)


def at512(index):
    return pl.ds(pl.multiple_of(index * 512, 512), 512)


HBM = pl.BlockSpec(memory_space=pltpu.HBM)
VMEM = pl.BlockSpec(memory_space=pltpu.VMEM)
SMEM = pl.BlockSpec(memory_space=pltpu.SMEM)


def call(kernel, ins, outs, scratch, flops, mib, raw=0, me=True):
    return pl.pallas_call(
        kernel,
        in_specs=[SMEM] * me + [VMEM] * (len(ins) - me - raw) + [HBM] * raw,
        out_specs=[VMEM] * len(outs),
        out_shape=[jax.ShapeDtypeStruct(s, d) for s, d in outs],
        scratch_shapes=[pltpu.VMEM(s, d) for s, d in scratch]
        + [pltpu.SemaphoreType.DMA((raw,))] * (raw > 0),
        compiler_params=pltpu.CompilerParams(vmem_limit_bytes=mib * 1024 * 1024),
        cost_estimate=pl.CostEstimate(
            flops=flops, bytes_accessed=1 << 20, transcendentals=0
        ),
    )(*ins)


def join_kernel(*refs):
    out = refs[-1]
    rows = out.shape[0] // (len(refs) - 1)
    for n, ref in enumerate(refs[:-1]):
        out[n * rows : (n + 1) * rows] = ref[...]


def join(parts):
    shape = (len(parts) * parts[0].shape[0],) + parts[0].shape[1:]
    return call(join_kernel, parts, [(shape, parts[0].dtype)], [], 1 << 20, 12, me=False)[0]


def join_split_kernel(low, high, left, right):
    for n, ref in enumerate((low, high)):
        rows = slice(n * 512, n * 512 + 512)
        left[rows, :] = ref[:, :768]
        right[rows, :] = ref[:, 768:]


def join_io_kernel(low, high, in_full, out_own):
    for p, j in enumerate(places(THREE)):
        ref, rows = (low, high)[p >> 3], lanes(p & 7)
        in_full[lanes(j), :] = ref[rows, :128]
        out_own[:, lanes(j)] = ref[rows, 128:]


def doubled(held, order):
    for n, step in enumerate(order):
        parts = [held, cross(held, step)]
        if n < len(order) - 1:
            held = join(parts)
    return parts


def apart(parts):
    outs = [((1024, 768), BF16), ((1024, 384), BF16)]
    return call(join_split_kernel, parts, outs, [], 1 << 20, 12, me=False)


def chunks(count, rows, body):
    def step(n, _):
        body(pl.ds(pl.multiple_of(n * rows, rows), rows))
        return 0

    lax.fori_loop(0, count, step, 0)


def prep_kernel(out_scale, down_scale, *rest):
    sources, (mine, theirs, io, one, two), held = rest[:6], rest[6:11], rest[11:]
    tokens, w_in, w_out, gate, up, down, sems = held
    c = lax.axis_index("c")
    copies = [
        pltpu.make_async_copy(a, b, sems.at[n]) for n, (a, b) in enumerate(zip(sources, held))
    ]
    for copy in copies:
        copy.start()
    for copy in copies:
        copy.wait()
    one[:, :768] = gate[...].astype(BF16)
    two[:, :768] = up[...].astype(BF16)
    for n in range(6):
        block = down[lanes(n), :].astype(BF16).astype(F32) * down_scale[...]
        (one, two)[n // 3][:, 768 + n % 3 * 128 : 896 + n % 3 * 128] = block.astype(BF16)
    io[:, :128] = w_in[...].astype(BF16)
    io[:, 128:] = (w_out[...].astype(BF16).astype(F32) * out_scale[...]).astype(BF16)
    mine[...] = tokens[at512(c), :]
    theirs[...] = tokens[at512(1 - c), :]


def turn_gain(me, gain, turned):
    for j in range(16):
        turned[:, lanes(j)] = gain[:, at128(me[0] ^ xor_of(j, me[2]))]


def channels_kernel(me, gain, in_own, in_other, t0, t1, t2, t3, *outs):
    own, other, tokens, turned, weights = outs
    f, t, c = me[0], me[1], me[2]
    turn_gain(me, gain, turned)
    a = jnp.where(c == 0, 2, 6)
    for ref, base in ((t0, 0), (t1, a), (t2, a ^ 4), (t3, 4)):
        for n in range(2):
            for h in range(2):
                j = block_of(((t ^ base ^ n) * 2 + h) ^ f, c)
                tokens[:, at128(j)] = ref[n, :, lanes(h)]
    for j in range(16):
        weights[lanes(j), :128] = in_own[lanes(j), :]
        weights[lanes(other_core(j)), 128:] = in_other[lanes(j), :]

    def body(rows):
        x = tokens[rows, :].astype(F32)
        squares = jnp.sum(x * x, axis=1, keepdims=True)
        inverse = lax.rsqrt(squares / D + EPSILON)
        scaled = (x * turned[...]).astype(BF16)
        total = jnp.dot(scaled, weights[...], preferred_element_type=F32) * inverse
        own[rows, :] = total[:, :128]
        other[rows, :] = total[:, 128:]

    chunks(4, 128, body)


def pooling_kernel(me, mine, theirs, scale, out_mine, out_theirs, ch, across, running, held):
    t, c = me[1], me[2]
    window = jnp.left_shift(2, t >> 1)
    half = window // 2
    ch[at512(c), :] = mine[...] * scale[...]
    ch[at512(1 - c), :] = theirs[...] * scale[...]

    p = lax.broadcasted_iota(jnp.int32, (256, 256), 0)
    q = lax.broadcasted_iota(jnp.int32, (256, 256), 1)
    inside = (q >= p - half) & (q < p + (window - half)) & (p // GRID_W == q // GRID_W)
    band = jnp.where(inside, 1.0, 0.0).astype(BF16)
    for n in range(4):
        rows = slice(n * 256, n * 256 + 256)
        values = ch[rows, :]
        high = values.astype(BF16)
        low = (values - high.astype(F32)).astype(BF16)
        both = jnp.concatenate([high, low], axis=1)
        sums = jnp.dot(band, both, preferred_element_type=F32)
        across[rows, :] = sums[:, :128] + sums[:, 128:]

    total = jnp.zeros((GRID_W, 128), F32)
    running[0] = total
    for n in range(ROWS):
        total = total + across[n * GRID_W : n * GRID_W + GRID_W, :]
        running[n + 1] = total
    column = lax.broadcasted_iota(jnp.int32, (GRID_W, 128), 0)
    wide = jnp.minimum(column + (window - half), GRID_W) - jnp.maximum(column - half, 0)
    wide = wide.astype(F32)
    for n in range(ROWS):
        upper = jnp.minimum(n + (window - half), ROWS)
        lower = jnp.maximum(n - half, 0)
        sums = running[upper] - running[lower]
        rows = slice(n * GRID_W, n * GRID_W + GRID_W)
        cells = wide * (upper - lower).astype(F32)
        held[rows, :] = (sums / cells - ch[rows, :]).astype(BF16)
    out_mine[...] = held[at512(c), :]
    out_theirs[...] = held[at512(1 - c), :]


def residual_kernel(me, tokens, *rest):
    pooled, own, residual = rest[:4], rest[4:8], rest[12]
    other = (rest[8], rest[10], rest[9], rest[11])

    def body(rows):
        pairs = [jnp.concatenate([p[0, rows, :], p[1, rows, :]], axis=1) for p in pooled]
        for n in range(4):
            columns = slice(n * 512, n * 512 + 512)
            mixed = tokens[rows, columns].astype(F32)
            for pair, a, b in zip(pairs, own, other):
                seats = [other_core(j) for j in range(n * 4, n * 4 + 4)]
                lower = jnp.concatenate([b[:, lanes(j)] for j in seats], axis=1)
                weights = jnp.concatenate([a[:, columns], lower], axis=0)
                mixed = mixed + jnp.dot(pair, weights, preferred_element_type=F32)
            residual[rows, columns] = mixed.astype(BF16)

    chunks(2, 256, body)


def hidden_kernel(theirs, me, residual, gain, gs, us, g0, g1, u0, u1, hidden, own, turned):
    f, t, c = me[0], me[1], me[2]
    seat = other_core if theirs else (lambda j: j)
    turn_gain(me, gain, turned)
    holder = 1 - c if theirs else c
    for h in range(2):
        own[:, lanes(h)] = residual[:, at128(block_of((t * 2 + h) ^ f, holder))]

    def body(rows):
        wide = residual[rows, :].astype(F32)
        squares = jnp.sum(wide * wide, axis=1, keepdims=True)
        inverse = lax.rsqrt(squares / D + EPSILON)
        blocks = [
            (wide[:, lanes(seat(j))] * turned[:, lanes(j)]).astype(BF16) for j in range(16)
        ]

        def product(order, low, high):
            spots = places(order)
            left = jnp.concatenate([blocks[j] for j in spots[:8]], axis=1)
            right = jnp.concatenate([blocks[j] for j in spots[8:]], axis=1)
            total = jnp.dot(left, low[...], preferred_element_type=F32)
            return total + jnp.dot(right, high[...], preferred_element_type=F32)

        gate = product(ONE, g0, g1) * inverse * gs[...]
        up = product(TWO, u0, u1) * inverse * us[...]
        hidden[rows, :] = (gate / (1.0 + jnp.exp(-gate)) * up).astype(BF16)

    chunks(2, 256, body)


def products(slot, me, held, d0, d1, e0, e1, keep, send, weights):
    f, t, c = me[0], me[1], me[2]
    a, b = jnp.where(c == 0, 1, 3), jnp.where(c == 0, 3, 1)
    pair = ((2, 2), (a, b), (b, a), (0, 0))[slot]
    for core in range(2):
        for h in range(2):
            j = block_of(((t ^ (pair[core] * 2 + core)) * 2 + h) ^ f, c)
            for order, low, high, base in ((ONE, d0, d1, 0), (TWO, e0, e1, 384)):
                p = position(order, j)
                for k in range(3):
                    there = slice(base + k * 128, base + k * 128 + 128)
                    weights[there, lanes(core * 2 + h)] = jnp.where(
                        p < 8,
                        low[at128(p & 7), lanes(k)],
                        high[at128(p & 7), lanes(k)],
                    )
    both = jnp.dot(held[...], weights[...], preferred_element_type=F32)
    keep[...] = both[:, :256].astype(BF16)
    send[...] = both[:, 256:].astype(BF16)


def down_first_kernel(me, mine, theirs, own_mine, own_theirs, d0, d1, e0, e1, *outs):
    keep, send, held, own, weights = outs
    c = me[2]
    held[at512(c), :] = mine[...]
    held[at512(1 - c), :] = theirs[...]
    own[at512(c), :] = own_mine[...]
    own[at512(1 - c), :] = own_theirs[...]
    products(0, me, held, d0, d1, e0, e1, keep, send, weights)


def layer(
    tokens,
    mix_gain,
    in_weight,
    in_scale,
    out_weight,
    out_scale,
    ffn_gain,
    gate_weight,
    gate_scale,
    up_weight,
    up_scale,
    down_weight,
    down_scale,
):
    z, y, x, c = (lax.axis_index(a) for a in ("z", "y", "x", "c"))
    me = jnp.stack([z * 4 + y, x * 2 + c, c]).astype(jnp.int32)

    sources = [tokens, in_weight, out_weight, gate_weight, up_weight, down_weight]
    mine, theirs, io, one, two = call(
        prep_kernel,
        [
            out_scale[None],
            down_scale[None],
            *(pltpu.with_memory_space_constraint(v, pltpu.HBM) for v in sources),
        ],
        [((512, 256), BF16)] * 2 + [((128, 256), BF16)] + [((128, 1152), BF16)] * 2,
        [(v.shape, v.dtype) for v in sources],
        1 << 22,
        12,
        raw=len(sources),
        me=False,
    )

    gate_held, down_one_held = apart(doubled(one, ONE[:3]))
    up_held, down_two_held = apart(doubled(two, TWO[:3]))
    gate, up = cross(gate_held, ONE[3]), cross(up_held, TWO[3])
    columns = [down_one_held, cross(down_one_held, ONE[3])]
    columns += [down_two_held, cross(down_two_held, TWO[3])]
    in_full, out_own = call(
        join_io_kernel,
        doubled(io, THREE),
        [((D, 128), BF16), ((128, D), BF16)],
        [],
        1 << 20,
        12,
        me=False,
    )

    pieces = spread(join([mine[None], swap(theirs)[None]]))

    outs = spread(out_own)
    own, other, half_tokens = call(
        channels_kernel,
        [me, mix_gain[None], in_full, swap(in_full), *pieces],
        [((512, 128), F32), ((512, 128), F32), ((512, D), BF16)],
        [((1, D), F32), ((D, 256), BF16)],
        2 * 512 * D * 256,
        20,
    )
    mine, theirs = call(
        pooling_kernel,
        [me, own, swap(other), in_scale[None]],
        [((512, 128), BF16)] * 2,
        [
            ((1024, 128), F32),
            ((1024, 128), F32),
            ((ROWS + 1, GRID_W, 128), F32),
            ((1024, 128), BF16),
        ],
        2 * 1024 * 256 * 256,
        8,
    )
    pooled = spread(join([mine[None], swap(theirs)[None]]))
    (residual,) = call(
        residual_kernel,
        [
            me,
            half_tokens,
            *pooled,
            *outs,
            *(swap(w) for w in outs),
        ],
        [((512, D), BF16)],
        [],
        2 * 512 * 1024 * D,
        20,
    )

    widening = [gate_held, gate, up_held, up]

    def hidden_of(theirs, rows):
        return call(
            functools.partial(hidden_kernel, theirs),
            [me, rows, ffn_gain[None], gate_scale[None], up_scale[None], *widening],
            [((512, 768), BF16), ((512, 256), BF16)],
            [((1, D), F32)],
            2 * 512 * 1536 * D,
            24,
        )

    hidden, kept = hidden_of(False, residual)
    hidden_b, kept_b = hidden_of(True, swap(residual))
    sums = [((1024, 256), BF16)] * 2
    keep, send, held, kept = call(
        down_first_kernel,
        [me, hidden, hidden_b, kept, kept_b, *columns],
        sums + [((1024, 768), BF16), ((1024, 256), BF16)],
        [((768, 512), BF16)],
        2 * 1024 * 768 * 512,
        20,
    )
    keeps, gots = [keep], [swap(send)]
    for n in range(1, 4):
        keep, send = call(
            functools.partial(products, n),
            [me, held, *columns],
            sums,
            [((768, 512), BF16)],
            2 * 1024 * 768 * 512,
            16,
        )
        keeps.append(keep)
        gots.append(swap(send))

    chip = [k.astype(F32) + g.astype(F32) for k, g in zip(keeps, gots)]
    passed = cross(chip[0].astype(BF16), "xa").astype(F32)
    came = cross(chip[1].astype(BF16), "xa").astype(F32)
    last = cross((chip[2] + passed).astype(BF16), "xb").astype(F32)
    return (kept.astype(F32) + (chip[3] + came + last)).astype(BF16)


def solution(mesh):
    finer = Mesh(mesh.devices.reshape(4, 4, 4, 2), ("z", "y", "x", "c"))
    return jax.shard_map(
        layer,
        mesh=finer,
        in_specs=(
            P(FS, TP),
            P(),
            P(FS, TP),
            P(TP),
            P(TP, FS),
            P(FS),
            P(),
            P(FS, TP),
            P(TP),
            P(FS, TP),
            P(TP),
            P(TP, FS),
            P(FS),
        ),
        out_specs=P(FS, TP),
        check_vma=False,
    )
```

```python
import functools

import jax
import jax.numpy as jnp
from jax import lax
from jax.experimental import pallas as pl
from jax.experimental.pallas import tpu as pltpu
from jax.sharding import Mesh
from jax.sharding import PartitionSpec as P

D = 2048
GRID_W = 64
ROWS = 16
EPSILON = 1e-06
FS = ("z", "y")
TP = ("x", "c")
BF16 = jnp.bfloat16
F32 = jnp.float32


BIT = {"ya": 0, "yb": 1, "za": 2, "zb": 3}
ONE = ("ya", "za", "yb", "zb")
TWO = ("za", "yb", "zb", "ya")
THREE = ("yb", "za", "ya", "zb")


def mask_of(step, c):
    if step[1:] == "ab":
        return 2
    return 1 if (step[-1] == "a") == (c == 0) else 3


def cross(value, step):
    axis = step[0]
    pairs = [(i * 2 + c, (i ^ mask_of(step, c)) * 2 + c) for i in range(4) for c in range(2)]
    return lax.ppermute(value, (axis, "c"), pairs)


def swap(value):
    return lax.ppermute(value, "c", [(0, 1), (1, 0)])


def spread(held):
    a = cross(held, "xa")
    b = cross(held, "xb")
    return [held, a, b, cross(a, "xb")]


def places(order):
    return [sum(((p >> k) & 1) << BIT[s] for k, s in enumerate(order)) for p in range(16)]


def position(order, block):
    total = 0
    for k, step in enumerate(order):
        total = total + (((block >> BIT[step]) & 1) << k)
    return total


def xor_of(j, c):
    values = []
    for core in range(2):
        value = 0
        for step, bit in BIT.items():
            if (j >> bit) & 1:
                value ^= mask_of(step, core) * (4 if step[0] == "z" else 1)
        values.append(value)
    return values[0] + c * (values[1] - values[0])


def block_of(xor, c):
    high = (xor >> 1) & 5
    low = (xor ^ (xor >> 1)) & 5
    return jnp.where(c == 0, high * 2 + low, low * 2 + high)


def other_core(j):
    return ((j & 5) << 1) | ((j >> 1) & 5)


def lanes(j):
    return slice(j * 128, j * 128 + 128)


def at128(index):
    return pl.ds(pl.multiple_of(index * 128, 128), 128)


def at512(index):
    return pl.ds(pl.multiple_of(index * 512, 512), 512)


HBM = pl.BlockSpec(memory_space=pltpu.HBM)
VMEM = pl.BlockSpec(memory_space=pltpu.VMEM)
SMEM = pl.BlockSpec(memory_space=pltpu.SMEM)


def call(kernel, ins, outs, scratch, flops, mib, raw=0, me=True):
    return pl.pallas_call(
        kernel,
        in_specs=[SMEM] * me + [VMEM] * (len(ins) - me - raw) + [HBM] * raw,
        out_specs=[VMEM] * len(outs),
        out_shape=[jax.ShapeDtypeStruct(s, d) for s, d in outs],
        scratch_shapes=[pltpu.VMEM(s, d) for s, d in scratch]
        + [pltpu.SemaphoreType.DMA((raw,))] * (raw > 0),
        compiler_params=pltpu.CompilerParams(vmem_limit_bytes=mib * 1024 * 1024),
        cost_estimate=pl.CostEstimate(
            flops=flops, bytes_accessed=1 << 20, transcendentals=0
        ),
    )(*ins)


def join_kernel(*refs):
    out = refs[-1]
    rows = out.shape[0] // (len(refs) - 1)
    for n, ref in enumerate(refs[:-1]):
        out[n * rows : (n + 1) * rows] = ref[...]


def join(parts):
    shape = (len(parts) * parts[0].shape[0],) + parts[0].shape[1:]
    return call(join_kernel, parts, [(shape, parts[0].dtype)], [], 1 << 20, 12, me=False)[0]


def split_kernel(held, came, left_came, right_out):
    left_came[...] = came[:, :768]
    right_out[:512, :] = held[:, 768:]
    right_out[512:, :] = came[:, 768:]


def join_io_kernel(low, high, in_full, out_own):
    for p, j in enumerate(places(THREE)):
        ref, rows = (low, high)[p >> 3], lanes(p & 7)
        in_full[lanes(j), :] = ref[rows, :128]
        out_own[:, lanes(j)] = ref[rows, 128:]


def doubled(held, order):
    for n, step in enumerate(order):
        parts = [held, cross(held, step)]
        if n < len(order) - 1:
            held = join(parts)
    return parts


def sequence(block, order):
    held = join(doubled(block, order[:2]))
    left = held[:, :768]
    came = cross(held, order[2])
    first = cross(left, order[3])
    outs = [((512, 768), BF16), ((1024, 384), BF16)]
    left_came, right = call(split_kernel, [held, came], outs, [], 1 << 20, 12, me=False)
    second = cross(left_came, order[3])
    return [left, left_came, first, second], [right, cross(right, order[3])]


def chunks(count, rows, body):
    def step(n, _):
        body(pl.ds(pl.multiple_of(n * rows, rows), rows))
        return 0

    lax.fori_loop(0, count, step, 0)


def prep_kernel(*rest):
    sources, (mine, theirs, io, one, two), held = rest[:8], rest[8:13], rest[13:]
    tokens, w_in, w_out, gate, up, down, out_scale, down_scale, sems = held
    c = lax.axis_index("c")
    copies = [
        pltpu.make_async_copy(a, b, sems.at[n]) for n, (a, b) in enumerate(zip(sources, held))
    ]
    for copy in copies:
        copy.start()
    for copy in copies:
        copy.wait()
    one[:, :768] = gate[...].astype(BF16)
    two[:, :768] = up[...].astype(BF16)
    for n in range(6):
        block = down[lanes(n), :].astype(BF16).astype(F32) * down_scale[...]
        (one, two)[n // 3][:, 768 + n % 3 * 128 : 896 + n % 3 * 128] = block.astype(BF16)
    io[:, :128] = w_in[...].astype(BF16)
    io[:, 128:] = (w_out[...].astype(BF16).astype(F32) * out_scale[...]).astype(BF16)
    mine[...] = tokens[at512(c), :]
    theirs[...] = tokens[at512(1 - c), :]


def turn_gain(me, gain, turned):
    for j in range(16):
        turned[:, lanes(j)] = gain[:, at128(me[0] ^ xor_of(j, me[2]))]


def channels_kernel(me, gain, in_own, in_other, t0, t1, t2, t3, *outs):
    own, other, tokens, turned, weights = outs
    f, t, c = me[0], me[1], me[2]
    turn_gain(me, gain, turned)
    a = jnp.where(c == 0, 2, 6)
    for ref, base in ((t0, 0), (t1, a), (t2, a ^ 4), (t3, 4)):
        for n in range(2):
            for h in range(2):
                j = block_of(((t ^ base ^ n) * 2 + h) ^ f, c)
                tokens[:, at128(j)] = ref[n, :, lanes(h)]
    for j in range(16):
        weights[lanes(j), :128] = in_own[lanes(j), :]
        weights[lanes(other_core(j)), 128:] = in_other[lanes(j), :]

    def body(rows):
        x = tokens[rows, :].astype(F32)
        squares = jnp.sum(x * x, axis=1, keepdims=True)
        inverse = lax.rsqrt(squares / D + EPSILON)
        scaled = (x * turned[...]).astype(BF16)
        total = jnp.dot(scaled, weights[...], preferred_element_type=F32) * inverse
        own[rows, :] = total[:, :128]
        other[rows, :] = total[:, 128:]

    chunks(4, 128, body)


def pooling_kernel(me, mine, theirs, scale, out_mine, out_theirs, ch, across, running, held):
    t, c = me[1], me[2]
    window = jnp.left_shift(2, t >> 1)
    half = window // 2
    ch[at512(c), :] = mine[...] * scale[...]
    ch[at512(1 - c), :] = theirs[...] * scale[...]

    p = lax.broadcasted_iota(jnp.int32, (256, 256), 0)
    q = lax.broadcasted_iota(jnp.int32, (256, 256), 1)
    inside = (q >= p - half) & (q < p + (window - half)) & (p // GRID_W == q // GRID_W)
    band = jnp.where(inside, 1.0, 0.0).astype(BF16)
    for n in range(4):
        rows = slice(n * 256, n * 256 + 256)
        values = ch[rows, :]
        high = values.astype(BF16)
        low = (values - high.astype(F32)).astype(BF16)
        both = jnp.concatenate([high, low], axis=1)
        sums = jnp.dot(band, both, preferred_element_type=F32)
        across[rows, :] = sums[:, :128] + sums[:, 128:]

    total = jnp.zeros((GRID_W, 128), F32)
    running[0] = total
    for n in range(ROWS):
        total = total + across[n * GRID_W : n * GRID_W + GRID_W, :]
        running[n + 1] = total
    column = lax.broadcasted_iota(jnp.int32, (GRID_W, 128), 0)
    wide = jnp.minimum(column + (window - half), GRID_W) - jnp.maximum(column - half, 0)
    wide = wide.astype(F32)
    for n in range(ROWS):
        upper = jnp.minimum(n + (window - half), ROWS)
        lower = jnp.maximum(n - half, 0)
        sums = running[upper] - running[lower]
        rows = slice(n * GRID_W, n * GRID_W + GRID_W)
        cells = wide * (upper - lower).astype(F32)
        held[rows, :] = (sums / cells - ch[rows, :]).astype(BF16)
    out_mine[...] = held[at512(c), :]
    out_theirs[...] = held[at512(1 - c), :]


def residual_kernel(me, tokens, *rest):
    pooled, own, residual = rest[:4], rest[4:8], rest[12]
    other = (rest[8], rest[10], rest[9], rest[11])

    def body(rows):
        pairs = [jnp.concatenate([p[0, rows, :], p[1, rows, :]], axis=1) for p in pooled]
        for n in range(4):
            columns = slice(n * 512, n * 512 + 512)
            mixed = tokens[rows, columns].astype(F32)
            for pair, a, b in zip(pairs, own, other):
                seats = [other_core(j) for j in range(n * 4, n * 4 + 4)]
                lower = jnp.concatenate([b[:, lanes(j)] for j in seats], axis=1)
                weights = jnp.concatenate([a[:, columns], lower], axis=0)
                mixed = mixed + jnp.dot(pair, weights, preferred_element_type=F32)
            residual[rows, columns] = mixed.astype(BF16)

    chunks(2, 256, body)


def hidden_kernel(theirs, me, residual, gain, gs, us, *rest):
    gates, ups, (hidden, own, turned) = rest[:4], rest[4:8], rest[8:]
    f, t, c = me[0], me[1], me[2]
    seat = other_core if theirs else (lambda j: j)
    turn_gain(me, gain, turned)
    holder = 1 - c if theirs else c
    for h in range(2):
        own[:, lanes(h)] = residual[:, at128(block_of((t * 2 + h) ^ f, holder))]

    def body(rows):
        wide = residual[rows, :].astype(F32)
        squares = jnp.sum(wide * wide, axis=1, keepdims=True)
        inverse = lax.rsqrt(squares / D + EPSILON)
        blocks = [
            (wide[:, lanes(seat(j))] * turned[:, lanes(j)]).astype(BF16) for j in range(16)
        ]

        def product(order, parts):
            left = jnp.concatenate([blocks[j] for j in places(order)], axis=1)
            weights = jnp.concatenate([part[...] for part in parts], axis=0)
            return jnp.dot(left, weights, preferred_element_type=F32)

        gate = product(ONE, gates) * inverse * gs[...]
        up = product(TWO, ups) * inverse * us[...]
        hidden[rows, :] = (gate / (1.0 + jnp.exp(-gate)) * up).astype(BF16)

    chunks(2, 256, body)


def products(slot, me, held, d0, d1, e0, e1, keep, send, weights):
    f, t, c = me[0], me[1], me[2]
    a, b = jnp.where(c == 0, 1, 3), jnp.where(c == 0, 3, 1)
    pair = ((2, 2), (a, b), (b, a), (0, 0))[slot]
    for core in range(2):
        for h in range(2):
            j = block_of(((t ^ (pair[core] * 2 + core)) * 2 + h) ^ f, c)
            for order, low, high, base in ((ONE, d0, d1, 0), (TWO, e0, e1, 384)):
                p = position(order, j)
                for k in range(3):
                    there = slice(base + k * 128, base + k * 128 + 128)
                    weights[there, lanes(core * 2 + h)] = jnp.where(
                        p < 8,
                        low[at128(p & 7), lanes(k)],
                        high[at128(p & 7), lanes(k)],
                    )
    both = jnp.dot(held[...], weights[...], preferred_element_type=F32)
    keep[...] = both[:, :256].astype(BF16)
    send[...] = both[:, 256:].astype(BF16)


def down_first_kernel(me, mine, theirs, own_mine, own_theirs, d0, d1, e0, e1, *outs):
    keep, send, held, own, weights = outs
    c = me[2]
    held[at512(c), :] = mine[...]
    held[at512(1 - c), :] = theirs[...]
    own[at512(c), :] = own_mine[...]
    own[at512(1 - c), :] = own_theirs[...]
    products(0, me, held, d0, d1, e0, e1, keep, send, weights)


def layer(
    tokens,
    mix_gain,
    in_weight,
    in_scale,
    out_weight,
    out_scale,
    ffn_gain,
    gate_weight,
    gate_scale,
    up_weight,
    up_scale,
    down_weight,
    down_scale,
):
    z, y, x, c = (lax.axis_index(a) for a in ("z", "y", "x", "c"))
    me = jnp.stack([z * 4 + y, x * 2 + c, c]).astype(jnp.int32)

    sources = [tokens, in_weight, out_weight, gate_weight, up_weight, down_weight]
    sources += [out_scale[None], down_scale[None]]
    mine, theirs, io, one, two = call(
        prep_kernel,
        [
            *(pltpu.with_memory_space_constraint(v, pltpu.HBM) for v in sources),
        ],
        [((512, 256), BF16)] * 2 + [((128, 256), BF16)] + [((128, 1152), BF16)] * 2,
        [(v.shape, v.dtype) for v in sources],
        1 << 22,
        12,
        raw=len(sources),
        me=False,
    )

    gate, columns = sequence(one, ONE)
    up, more = sequence(two, TWO)
    columns = columns + more
    in_full, out_own = call(
        join_io_kernel,
        doubled(io, THREE),
        [((D, 128), BF16), ((128, D), BF16)],
        [],
        1 << 20,
        12,
        me=False,
    )

    pieces = spread(join([mine[None], swap(theirs)[None]]))

    outs = spread(out_own)
    own, other, half_tokens = call(
        channels_kernel,
        [me, mix_gain[None], in_full, swap(in_full), *pieces],
        [((512, 128), F32), ((512, 128), F32), ((512, D), BF16)],
        [((1, D), F32), ((D, 256), BF16)],
        2 * 512 * D * 256,
        20,
    )
    mine, theirs = call(
        pooling_kernel,
        [me, own, swap(other), in_scale[None]],
        [((512, 128), BF16)] * 2,
        [
            ((1024, 128), F32),
            ((1024, 128), F32),
            ((ROWS + 1, GRID_W, 128), F32),
            ((1024, 128), BF16),
        ],
        2 * 1024 * 256 * 256,
        8,
    )
    pooled = spread(join([mine[None], swap(theirs)[None]]))
    (residual,) = call(
        residual_kernel,
        [
            me,
            half_tokens,
            *pooled,
            *outs,
            *(swap(w) for w in outs),
        ],
        [((512, D), BF16)],
        [],
        2 * 512 * 1024 * D,
        20,
    )

    def hidden_of(theirs, rows):
        return call(
            functools.partial(hidden_kernel, theirs),
            [me, rows, ffn_gain[None], gate_scale[None], up_scale[None], *gate, *up],
            [((512, 768), BF16), ((512, 256), BF16)],
            [((1, D), F32)],
            2 * 512 * 1536 * D,
            24,
        )

    hidden, kept = hidden_of(False, residual)
    hidden_b, kept_b = hidden_of(True, swap(residual))
    sums = [((1024, 256), BF16)] * 2
    keep, send, held, kept = call(
        down_first_kernel,
        [me, hidden, hidden_b, kept, kept_b, *columns],
        sums + [((1024, 768), BF16), ((1024, 256), BF16)],
        [((768, 512), BF16)],
        2 * 1024 * 768 * 512,
        20,
    )
    keeps, gots = [keep], [swap(send)]
    for n in range(1, 4):
        keep, send = call(
            functools.partial(products, n),
            [me, held, *columns],
            sums,
            [((768, 512), BF16)],
            2 * 1024 * 768 * 512,
            16,
        )
        keeps.append(keep)
        gots.append(swap(send))

    chip = [k.astype(F32) + g.astype(F32) for k, g in zip(keeps, gots)]
    passed = cross(chip[0].astype(BF16), "xa").astype(F32)
    came = cross(chip[1].astype(BF16), "xa").astype(F32)
    last = cross((chip[2] + passed).astype(BF16), "xb").astype(F32)
    return (kept.astype(F32) + (chip[3] + came + last)).astype(BF16)


def solution(mesh):
    finer = Mesh(mesh.devices.reshape(4, 4, 4, 2), ("z", "y", "x", "c"))
    return jax.shard_map(
        layer,
        mesh=finer,
        in_specs=(
            P(FS, TP),
            P(),
            P(FS, TP),
            P(TP),
            P(TP, FS),
            P(FS),
            P(),
            P(FS, TP),
            P(TP),
            P(FS, TP),
            P(TP),
            P(TP, FS),
            P(FS),
        ),
        out_specs=P(FS, TP),
        check_vma=False,
    )
```

```python
import functools

import jax
import jax.numpy as jnp
from jax import lax
from jax.experimental import pallas as pl
from jax.experimental.pallas import tpu as pltpu
from jax.sharding import Mesh
from jax.sharding import PartitionSpec as P

D = 2048
GRID_W = 64
ROWS = 16
EPSILON = 1e-06
FS = ("z", "y")
TP = ("x", "c")
BF16 = jnp.bfloat16
F32 = jnp.float32


BIT = {"ya": 0, "yb": 1, "za": 2, "zb": 3}
ONE = ("ya", "za", "yb", "zb")
TWO = ("za", "yb", "zb", "ya")
THREE = ("yb", "za", "ya", "zb")


def mask_of(step, c):
    if step[1:] == "ab":
        return 2
    return 1 if (step[-1] == "a") == (c == 0) else 3


def cross(value, step):
    axis = step[0]
    pairs = [(i * 2 + c, (i ^ mask_of(step, c)) * 2 + c) for i in range(4) for c in range(2)]
    return lax.ppermute(value, (axis, "c"), pairs)


def swap(value):
    return lax.ppermute(value, "c", [(0, 1), (1, 0)])


def spread(held):
    a = cross(held, "xa")
    b = cross(held, "xb")
    return [held, a, b, cross(a, "xb")]


def places(order):
    return [sum(((p >> k) & 1) << BIT[s] for k, s in enumerate(order)) for p in range(16)]


def position(order, block):
    total = 0
    for k, step in enumerate(order):
        total = total + (((block >> BIT[step]) & 1) << k)
    return total


def xor_of(j, c):
    values = []
    for core in range(2):
        value = 0
        for step, bit in BIT.items():
            if (j >> bit) & 1:
                value ^= mask_of(step, core) * (4 if step[0] == "z" else 1)
        values.append(value)
    return values[0] + c * (values[1] - values[0])


def block_of(xor, c):
    high = (xor >> 1) & 5
    low = (xor ^ (xor >> 1)) & 5
    return jnp.where(c == 0, high * 2 + low, low * 2 + high)


def other_core(j):
    return ((j & 5) << 1) | ((j >> 1) & 5)


def lanes(j):
    return slice(j * 128, j * 128 + 128)


def at128(index):
    return pl.ds(pl.multiple_of(index * 128, 128), 128)


def at512(index):
    return pl.ds(pl.multiple_of(index * 512, 512), 512)


HBM = pl.BlockSpec(memory_space=pltpu.HBM)
VMEM = pl.BlockSpec(memory_space=pltpu.VMEM)
SMEM = pl.BlockSpec(memory_space=pltpu.SMEM)


def call(kernel, ins, outs, scratch, flops, mib, raw=0, me=True):
    return pl.pallas_call(
        kernel,
        in_specs=[SMEM] * me + [VMEM] * (len(ins) - me - raw) + [HBM] * raw,
        out_specs=[VMEM] * len(outs),
        out_shape=[jax.ShapeDtypeStruct(s, d) for s, d in outs],
        scratch_shapes=[pltpu.VMEM(s, d) for s, d in scratch]
        + [pltpu.SemaphoreType.DMA((raw,))] * (raw > 0),
        compiler_params=pltpu.CompilerParams(vmem_limit_bytes=mib * 1024 * 1024),
        cost_estimate=pl.CostEstimate(
            flops=flops, bytes_accessed=1 << 20, transcendentals=0
        ),
    )(*ins)


def join_kernel(*refs):
    out = refs[-1]
    rows = out.shape[0] // (len(refs) - 1)
    for n, ref in enumerate(refs[:-1]):
        out[n * rows : (n + 1) * rows] = ref[...]


def join(parts):
    shape = (len(parts) * parts[0].shape[0],) + parts[0].shape[1:]
    return call(join_kernel, parts, [(shape, parts[0].dtype)], [], 1 << 20, 12, me=False)[0]


def split_kernel(held, came, left_came, right_out):
    left_came[...] = came[:, :768]
    right_out[:512, :] = held[:, 768:]
    right_out[512:, :] = came[:, 768:]


def join_io_kernel(low, high, in_full, out_own):
    for p, j in enumerate(places(THREE)):
        ref, rows = (low, high)[p >> 3], lanes(p & 7)
        in_full[lanes(j), :] = ref[rows, :128]
        out_own[:, lanes(j)] = ref[rows, 128:]


def doubled(held, order):
    for n, step in enumerate(order):
        parts = [held, cross(held, step)]
        if n < len(order) - 1:
            held = join(parts)
    return parts


def sequence(block, order):
    held = join(doubled(block, order[:2]))
    left = held[:, :768]
    came = cross(held, order[2])
    first = cross(left, order[3])
    outs = [((512, 768), BF16), ((1024, 384), BF16)]
    left_came, right = call(split_kernel, [held, came], outs, [], 1 << 20, 12, me=False)
    second = cross(left_came, order[3])
    return [left, left_came, first, second], [right, cross(right, order[3])]


def chunks(count, rows, body, flat=False):
    if flat:
        for n in range(count):
            body(slice(n * rows, n * rows + rows))
        return

    def step(n, _):
        body(pl.ds(pl.multiple_of(n * rows, rows), rows))
        return 0

    lax.fori_loop(0, count, step, 0)


def prep_kernel(*rest):
    sources, (mine, theirs, io, one, two), held = rest[:8], rest[8:13], rest[13:]
    tokens, w_in, w_out, gate, up, down, out_scale, down_scale, sems = held
    c = lax.axis_index("c")
    copies = [
        pltpu.make_async_copy(a, b, sems.at[n]) for n, (a, b) in enumerate(zip(sources, held))
    ]
    for copy in copies:
        copy.start()
    for copy in copies:
        copy.wait()
    one[:, :768] = gate[...].astype(BF16)
    two[:, :768] = up[...].astype(BF16)
    for n in range(6):
        block = down[lanes(n), :].astype(BF16).astype(F32) * down_scale[...]
        (one, two)[n // 3][:, 768 + n % 3 * 128 : 896 + n % 3 * 128] = block.astype(BF16)
    io[:, :128] = w_in[...].astype(BF16)
    io[:, 128:] = (w_out[...].astype(BF16).astype(F32) * out_scale[...]).astype(BF16)
    mine[...] = tokens[at512(c), :]
    theirs[...] = tokens[at512(1 - c), :]


def turn_gain(me, gain, turned):
    for j in range(16):
        turned[:, lanes(j)] = gain[:, at128(me[0] ^ xor_of(j, me[2]))]


def channels_kernel(me, gain, in_own, in_other, t0, t1, t2, t3, *outs):
    own, other, tokens, turned, weights = outs
    f, t, c = me[0], me[1], me[2]
    turn_gain(me, gain, turned)
    a = jnp.where(c == 0, 2, 6)
    for ref, base in ((t0, 0), (t1, a), (t2, a ^ 4), (t3, 4)):
        for n in range(2):
            for h in range(2):
                j = block_of(((t ^ base ^ n) * 2 + h) ^ f, c)
                tokens[:, at128(j)] = ref[n, :, lanes(h)]
    for j in range(16):
        weights[lanes(j), :128] = in_own[lanes(j), :]
        weights[lanes(other_core(j)), 128:] = in_other[lanes(j), :]

    def body(rows):
        x = tokens[rows, :].astype(F32)
        squares = jnp.sum(x * x, axis=1, keepdims=True)
        inverse = lax.rsqrt(squares / D + EPSILON)
        scaled = (x * turned[...]).astype(BF16)
        total = jnp.dot(scaled, weights[...], preferred_element_type=F32) * inverse
        own[rows, :] = total[:, :128]
        other[rows, :] = total[:, 128:]

    chunks(4, 128, body)


def pooling_kernel(me, mine, theirs, scale, out_mine, out_theirs, ch, across, running, held):
    t, c = me[1], me[2]
    window = jnp.left_shift(2, t >> 1)
    half = window // 2
    ch[at512(c), :] = mine[...] * scale[...]
    ch[at512(1 - c), :] = theirs[...] * scale[...]

    p = lax.broadcasted_iota(jnp.int32, (256, 256), 0)
    q = lax.broadcasted_iota(jnp.int32, (256, 256), 1)
    inside = (q >= p - half) & (q < p + (window - half)) & (p // GRID_W == q // GRID_W)
    band = jnp.where(inside, 1.0, 0.0).astype(BF16)
    for n in range(4):
        rows = slice(n * 256, n * 256 + 256)
        values = ch[rows, :]
        high = values.astype(BF16)
        low = (values - high.astype(F32)).astype(BF16)
        both = jnp.concatenate([high, low], axis=1)
        sums = jnp.dot(band, both, preferred_element_type=F32)
        across[rows, :] = sums[:, :128] + sums[:, 128:]

    total = jnp.zeros((GRID_W, 128), F32)
    running[0] = total
    for n in range(ROWS):
        total = total + across[n * GRID_W : n * GRID_W + GRID_W, :]
        running[n + 1] = total
    column = lax.broadcasted_iota(jnp.int32, (GRID_W, 128), 0)
    wide = jnp.minimum(column + (window - half), GRID_W) - jnp.maximum(column - half, 0)
    wide = wide.astype(F32)
    for n in range(ROWS):
        upper = jnp.minimum(n + (window - half), ROWS)
        lower = jnp.maximum(n - half, 0)
        sums = running[upper] - running[lower]
        rows = slice(n * GRID_W, n * GRID_W + GRID_W)
        cells = wide * (upper - lower).astype(F32)
        held[rows, :] = (sums / cells - ch[rows, :]).astype(BF16)
    out_mine[...] = held[at512(c), :]
    out_theirs[...] = held[at512(1 - c), :]


def residual_kernel(me, tokens, *rest):
    pooled, own, residual = rest[:4], rest[4:8], rest[12]
    other = (rest[8], rest[10], rest[9], rest[11])

    def body(rows):
        pairs = [jnp.concatenate([p[0, rows, :], p[1, rows, :]], axis=1) for p in pooled]
        for n in range(4):
            columns = slice(n * 512, n * 512 + 512)
            mixed = tokens[rows, columns].astype(F32)
            for pair, a, b in zip(pairs, own, other):
                seats = [other_core(j) for j in range(n * 4, n * 4 + 4)]
                lower = jnp.concatenate([b[:, lanes(j)] for j in seats], axis=1)
                weights = jnp.concatenate([a[:, columns], lower], axis=0)
                mixed = mixed + jnp.dot(pair, weights, preferred_element_type=F32)
            residual[rows, columns] = mixed.astype(BF16)

    chunks(1, 512, body, flat=True)


def hidden_kernel(theirs, me, residual, gain, gs, us, *rest):
    gates, ups, (hidden, own, turned) = rest[:4], rest[4:8], rest[8:]
    f, t, c = me[0], me[1], me[2]
    seat = other_core if theirs else (lambda j: j)
    turn_gain(me, gain, turned)
    holder = 1 - c if theirs else c
    for h in range(2):
        own[:, lanes(h)] = residual[:, at128(block_of((t * 2 + h) ^ f, holder))]

    def body(rows):
        wide = residual[rows, :].astype(F32)
        squares = jnp.sum(wide * wide, axis=1, keepdims=True)
        inverse = lax.rsqrt(squares / D + EPSILON)
        blocks = [
            (wide[:, lanes(seat(j))] * turned[:, lanes(j)]).astype(BF16) for j in range(16)
        ]

        def product(order, parts):
            left = jnp.concatenate([blocks[j] for j in places(order)], axis=1)
            weights = jnp.concatenate([part[...] for part in parts], axis=0)
            return jnp.dot(left, weights, preferred_element_type=F32)

        gate = product(ONE, gates) * inverse * gs[...]
        up = product(TWO, ups) * inverse * us[...]
        hidden[rows, :] = (gate / (1.0 + jnp.exp(-gate)) * up).astype(BF16)

    chunks(1, 512, body, flat=True)


def products(slot, me, held, d0, d1, e0, e1, keep, send, weights):
    f, t, c = me[0], me[1], me[2]
    a, b = jnp.where(c == 0, 1, 3), jnp.where(c == 0, 3, 1)
    pair = ((2, 2), (a, b), (b, a), (0, 0))[slot]
    for core in range(2):
        for h in range(2):
            j = block_of(((t ^ (pair[core] * 2 + core)) * 2 + h) ^ f, c)
            for order, low, high, base in ((ONE, d0, d1, 0), (TWO, e0, e1, 384)):
                p = position(order, j)
                for k in range(3):
                    there = slice(base + k * 128, base + k * 128 + 128)
                    weights[there, lanes(core * 2 + h)] = jnp.where(
                        p < 8,
                        low[at128(p & 7), lanes(k)],
                        high[at128(p & 7), lanes(k)],
                    )
    both = jnp.dot(held[...], weights[...], preferred_element_type=F32)
    keep[...] = both[:, :256].astype(BF16)
    send[...] = both[:, 256:].astype(BF16)


def down_first_kernel(me, mine, theirs, own_mine, own_theirs, d0, d1, e0, e1, *outs):
    keep, send, held, own, weights = outs
    c = me[2]
    held[at512(c), :] = mine[...]
    held[at512(1 - c), :] = theirs[...]
    own[at512(c), :] = own_mine[...]
    own[at512(1 - c), :] = own_theirs[...]
    products(0, me, held, d0, d1, e0, e1, keep, send, weights)


def layer(
    tokens,
    mix_gain,
    in_weight,
    in_scale,
    out_weight,
    out_scale,
    ffn_gain,
    gate_weight,
    gate_scale,
    up_weight,
    up_scale,
    down_weight,
    down_scale,
):
    z, y, x, c = (lax.axis_index(a) for a in ("z", "y", "x", "c"))
    me = jnp.stack([z * 4 + y, x * 2 + c, c]).astype(jnp.int32)

    sources = [tokens, in_weight, out_weight, gate_weight, up_weight, down_weight]
    sources += [out_scale[None], down_scale[None]]
    mine, theirs, io, one, two = call(
        prep_kernel,
        [
            *(pltpu.with_memory_space_constraint(v, pltpu.HBM) for v in sources),
        ],
        [((512, 256), BF16)] * 2 + [((128, 256), BF16)] + [((128, 1152), BF16)] * 2,
        [(v.shape, v.dtype) for v in sources],
        1 << 22,
        12,
        raw=len(sources),
        me=False,
    )

    gate, columns = sequence(one, ONE)
    up, more = sequence(two, TWO)
    columns = columns + more
    in_full, out_own = call(
        join_io_kernel,
        doubled(io, THREE),
        [((D, 128), BF16), ((128, D), BF16)],
        [],
        1 << 20,
        12,
        me=False,
    )

    pieces = spread(join([mine[None], swap(theirs)[None]]))

    outs = spread(out_own)
    own, other, half_tokens = call(
        channels_kernel,
        [me, mix_gain[None], in_full, swap(in_full), *pieces],
        [((512, 128), F32), ((512, 128), F32), ((512, D), BF16)],
        [((1, D), F32), ((D, 256), BF16)],
        2 * 512 * D * 256,
        20,
    )
    mine, theirs = call(
        pooling_kernel,
        [me, own, swap(other), in_scale[None]],
        [((512, 128), BF16)] * 2,
        [
            ((1024, 128), F32),
            ((1024, 128), F32),
            ((ROWS + 1, GRID_W, 128), F32),
            ((1024, 128), BF16),
        ],
        2 * 1024 * 256 * 256,
        8,
    )
    pooled = spread(join([mine[None], swap(theirs)[None]]))
    (residual,) = call(
        residual_kernel,
        [
            me,
            half_tokens,
            *pooled,
            *outs,
            *(swap(w) for w in outs),
        ],
        [((512, D), BF16)],
        [],
        2 * 512 * 1024 * D,
        20,
    )

    def hidden_of(theirs, rows):
        return call(
            functools.partial(hidden_kernel, theirs),
            [me, rows, ffn_gain[None], gate_scale[None], up_scale[None], *gate, *up],
            [((512, 768), BF16), ((512, 256), BF16)],
            [((1, D), F32)],
            2 * 512 * 1536 * D,
            24,
        )

    hidden, kept = hidden_of(False, residual)
    hidden_b, kept_b = hidden_of(True, swap(residual))
    sums = [((1024, 256), BF16)] * 2
    keep, send, held, kept = call(
        down_first_kernel,
        [me, hidden, hidden_b, kept, kept_b, *columns],
        sums + [((1024, 768), BF16), ((1024, 256), BF16)],
        [((768, 512), BF16)],
        2 * 1024 * 768 * 512,
        20,
    )
    keeps, gots = [keep], [swap(send)]
    for n in range(1, 4):
        keep, send = call(
            functools.partial(products, n),
            [me, held, *columns],
            sums,
            [((768, 512), BF16)],
            2 * 1024 * 768 * 512,
            16,
        )
        keeps.append(keep)
        gots.append(swap(send))

    chip = [k.astype(F32) + g.astype(F32) for k, g in zip(keeps, gots)]
    passed = cross(chip[0].astype(BF16), "xa").astype(F32)
    came = cross(chip[1].astype(BF16), "xa").astype(F32)
    last = cross((chip[2] + passed).astype(BF16), "xb").astype(F32)
    return (kept.astype(F32) + (chip[3] + came + last)).astype(BF16)


def solution(mesh):
    finer = Mesh(mesh.devices.reshape(4, 4, 4, 2), ("z", "y", "x", "c"))
    return jax.shard_map(
        layer,
        mesh=finer,
        in_specs=(
            P(FS, TP),
            P(),
            P(FS, TP),
            P(TP),
            P(TP, FS),
            P(FS),
            P(),
            P(FS, TP),
            P(TP),
            P(FS, TP),
            P(TP),
            P(TP, FS),
            P(FS),
        ),
        out_specs=P(FS, TP),
        check_vma=False,
    )
```
